32 devices in a mesh: grp: 2 (over x), ep: 8 (over z, y), tp: 2 (over core).
Axes of the slice: x: 2, y: 2, z: 4, core: 2. Of those that a mesh axis runs over, the one named last changes fastest.
Arguments:
- tokens: bfloat16 [4096, 2048], P(('grp', 'ep')), parts along dimension 0, may hold values from -6 to 6
- picks: int32 [8, 512], P(None, ('grp', 'ep')), parts along dimension 1, may hold values from 0 to 2047, as said below
- route_weights: bfloat16 [8, 512], P(None, ('grp', 'ep')), parts along dimension 1, may hold values from 0.19921875 to 1
- gate_weight: bfloat16 [8, 2048, 1024], P('ep', None, 'tp'), may hold values from -0.125 to 0.125
- up_weight: bfloat16 [8, 2048, 1024], P('ep', None, 'tp'), may hold values from -0.125 to 0.125
- down_weight: bfloat16 [8, 1024, 2048], P('ep', 'tp'), may hold values from -0.1875 to 0.1875
Outputs:
- mixed: bfloat16 [4096, 2048], P(('grp', 'ep'), 'tp'), parts along dimension 0
The draws below stay inside these ranges and needn't reach their ends.
There are 2 independent parts, one for each index of `grp`. The reference program is written for one: setup_inputs(seed, part) draws one part's arguments, and reference() takes and returns one part's arrays. A program takes and returns all parts, laid end to end along the dimension named above; an argument that names none is the same for every part. Nothing has to cross between parts.
Inputs may be any that keep to these rules, and one draw needn't show every extreme that they name: `picks`: slots k * 32 to (k + 1) * 32 - 1 of every expert name 32 different tokens of the block k * 256 to (k + 1) * 256 - 1.
All inputs are finite; a program needn't handle non-finite values.
Results may differ from the reference program's by a relative error of at most 0.0066.
Values may be sent and summed in bfloat16 or wider, within the bound.
A program may use at most 64 MiB of HBM per device.

```python
import jax
import jax.numpy as jnp
from jax import lax

D = 2048
FF = 1024
TOK_DEV = 256
PER = 32
EXPERTS = 8
CAP = 256
TOKENS = 2048
N_TP = 2


def draw_picks(key, part):
    sources = TOKENS // TOK_DEV
    keys = jax.random.split(jax.random.fold_in(key, 7), EXPERTS * sources)
    chosen = jax.vmap(lambda single: jax.random.permutation(single, TOK_DEV)[:PER])(keys)
    offsets = jnp.arange(sources, dtype=jnp.int32) * TOK_DEV
    chosen = chosen.astype(jnp.int32).reshape(EXPERTS, sources, PER) + offsets[None, :, None]
    return chosen.reshape(EXPERTS, sources * PER).astype(jnp.int32)


def block_levels(rng, extent, pieces, low, largest):
    level, own = 1.0, jax.random.fold_in(rng, 6)
    for axis_at, blocks in pieces:
        steps = jnp.exp(jax.random.uniform(jax.random.fold_in(own, axis_at), (blocks,), jnp.float32, low / len(pieces), largest / len(pieces)))
        level = level * jnp.repeat(steps, extent[axis_at] // blocks).reshape([-1 if axis == axis_at else 1 for axis in range(len(extent))])
    return level


def noise(rng, shape, scale, most, pieces=(), kind=jnp.bfloat16):
    loudness = block_levels(rng, shape, pieces, -0.22, 0.18) if pieces else 1.0
    array = jax.random.normal(rng, shape, jnp.float32) * scale * loudness
    return jnp.minimum(jnp.maximum(array, -most), most).astype(kind)


def setup_inputs(seed: int = 0, part: int = 0) -> dict:
    streams_of = jax.random.split(jax.random.key(seed), 7)
    part_splits = jax.random.split(jax.random.fold_in(streams_of[6], part), 7)
    tokens = noise(part_splits[0], (TOKENS, D), 1.0, 6.0, ((0, 8),))
    picks = draw_picks(jax.random.fold_in(jax.random.fold_in(streams_of[6], part), 71), part)
    route_weights = jnp.clip(0.19921875 + 0.80078125 * jax.random.uniform(part_splits[2], (EXPERTS, CAP), jnp.float32) ** block_levels(part_splits[2], (EXPERTS, CAP), ((1, 8),), -0.2, 0.2), 0.19921875, 1.0).astype(jnp.bfloat16)
    gate_weight = noise(streams_of[3], (EXPERTS, D, FF), D ** -0.5, 0.125, ((0, 8), (2, 2)))
    up_weight = noise(streams_of[4], (EXPERTS, D, FF), D ** -0.5, 0.125, ((0, 8), (2, 2)))
    down_weight = noise(streams_of[5], (EXPERTS, FF, D), FF ** -0.5, 0.1875, ((0, 8), (1, 2)))
    return dict(tokens=tokens, picks=picks, route_weights=route_weights, gate_weight=gate_weight, up_weight=up_weight, down_weight=down_weight)


def reference(tokens, picks, route_weights, gate_weight, up_weight, down_weight):
    half_width = FF // N_TP

    def one_expert(total, index):
        rows = jnp.take(tokens, picks[index], axis=0)
        gate = jnp.dot(rows, gate_weight[index], preferred_element_type=jnp.float32)
        up = jnp.dot(rows, up_weight[index], preferred_element_type=jnp.float32)
        scale = route_weights[index].astype(jnp.float32)[:, None]
        hidden = (jax.nn.silu(gate) * up * scale).astype(jnp.bfloat16)
        summed = jnp.zeros((rows.shape[0], D), jnp.float32)
        for block in range(N_TP):
            left = hidden[:, block * half_width:(block + 1) * half_width]
            right = down_weight[index, block * half_width:(block + 1) * half_width]
            partial_value = jnp.dot(left, right, preferred_element_type=jnp.float32).astype(jnp.bfloat16)
            summed = summed + partial_value.astype(jnp.float32)
        result = summed.astype(jnp.bfloat16).astype(jnp.float32)
        return total.at[picks[index]].add(result), None

    start = jnp.zeros((TOKENS, D), jnp.float32)
    total, _ = lax.scan(one_expert, start, jnp.arange(EXPERTS, dtype=jnp.int32))
    return total.astype(jnp.bfloat16)
```

```python
import functools

import jax
import jax.numpy as jnp
from jax import lax
from jax.experimental import pallas as pl
from jax.experimental.pallas import tpu as pltpu
from jax.sharding import PartitionSpec as P

MESH = pl.DeviceIdType.MESH
F32 = jnp.float32
BF16 = jnp.bfloat16


def flip(me, k):
    bit, out = 1, me
    while bit <= k:
        if k & bit:
            out = out + bit * (1 - 2 * ((me // bit) % 2))
        bit *= 2
    return out


def groups_of(n):
    if n < 4:
        return [list(range(n))]
    half, quarter = n // 2, n // 4
    return [
        list(range(half, half + quarter)),
        list(range(half)),
        list(range(half + quarter, n)),
    ]


def kernel(
    n, per, groups,
    tokens_hbm, ids_ref, half_ids_ref, route_ref, gate_hbm, up_hbm, down_hbm, out_ref,
    tokens, gate_w, up_w, down_w, outgoing, rows, mine, part_out, part_in, result, returned,
    load_sem, disp_send, disp_recv, fwd_send, fwd_recv, part_send, part_recv, ret_send, ret_recv,
):
    me, core = lax.axis_index("ep"), lax.axis_index("tp")
    other = 1 - core
    half = per // 2
    tok, width = tokens.shape
    cols = width // 2
    order = [k for g in groups for k in g]
    place = {k: i for i, k in enumerate(order)}

    loads = [
        pltpu.make_async_copy(src, dst, load_sem.at[i])
        for i, (src, dst) in enumerate(
            ((tokens_hbm, tokens), (gate_hbm.at[0], gate_w), (up_hbm.at[0], up_w), (down_hbm.at[0], down_w))
        )
    ]
    for load in loads:
        load.start()

    barrier = pltpu.get_barrier_semaphore()
    for k in order:
        if k:
            pl.semaphore_signal(barrier, inc=1, device_id={"ep": flip(me, k)}, device_id_type=MESH)
    pl.semaphore_signal(barrier, inc=1, device_id={"tp": other}, device_id_type=MESH)

    ids = jnp.where(core == 0, half_ids_ref[0:1, :], half_ids_ref[1:2, :])
    spots = lax.broadcasted_iota(jnp.int32, (tok, n * half), 0)
    pick = jnp.where(spots == ids, 1.0, 0.0).astype(BF16)
    loads[0].wait()
    outgoing[...] = lax.dot_general(
        pick, tokens[...], (((0,), (0,)), ((), ())), preferred_element_type=F32
    ).astype(BF16)

    def spot(k):
        return pl.ds(place[k] * per + pl.multiple_of(core * half, half), half)

    def dispatch(k):
        peer = flip(me, k)
        return pltpu.make_async_remote_copy(
            outgoing.at[pl.ds(pl.multiple_of(peer * half, half), half)], rows.at[spot(k)],
            disp_send.at[k], disp_recv.at[k], device_id={"ep": peer}, device_id_type=MESH,
        )

    def forward(k):
        src = rows.at[spot(k)] if k else outgoing.at[pl.ds(pl.multiple_of(me * half, half), half)]
        return pltpu.make_async_remote_copy(
            src, rows.at[spot(k)], fwd_send.at[k], fwd_recv.at[k], device_id={"tp": other}, device_id_type=MESH,
        )

    def swap(g):
        at = pl.ds(place[groups[g][0]] * per, len(groups[g]) * per)
        return pltpu.make_async_remote_copy(
            part_out.at[at], part_in.at[at], part_send.at[g], part_recv.at[g],
            device_id={"tp": other}, device_id_type=MESH,
        )

    def giveback(k):
        return pltpu.make_async_remote_copy(
            result.at[pl.ds(place[k] * per, per)], returned.at[pl.ds(pl.multiple_of(me * per, per), per)],
            ret_send.at[k], ret_recv.at[k], device_id={"ep": flip(me, k)}, device_id_type=MESH,
        )

    pl.semaphore_wait(barrier, n)
    for k in order:
        if k:
            dispatch(k).start()
    forward(0).start()
    rows[spot(0), :] = outgoing[pl.ds(pl.multiple_of(me * half, half), half), :]

    def relay(g):
        for k in groups[g]:
            if k:
                dispatch(k).wait_recv()
                forward(k).start()

    def compute(g):
        for k in groups[g]:
            forward(k).wait_recv()
        if g == 0:
            for load in loads[1:]:
                load.wait()
        count = len(groups[g]) * per
        at = pl.ds(place[groups[g][0]] * per, count)
        x = rows[at, :]
        gate = jnp.dot(x, gate_w[...], preferred_element_type=F32)
        up = jnp.dot(x, up_w[...], preferred_element_type=F32)
        hidden = (gate / (1.0 + jnp.exp(-gate)) * up).astype(BF16)
        theirs = down_w[:, pl.ds(pl.multiple_of(other * cols, cols), cols)]
        part_out[at, :] = jnp.dot(hidden, theirs, preferred_element_type=F32).astype(BF16)
        swap(g).start()
        ours = down_w[:, pl.ds(pl.multiple_of(core * cols, cols), cols)]
        mine[at, :] = jnp.dot(hidden, ours, preferred_element_type=F32)

    def finish(g):
        swap(g).wait_recv()
        at = pl.ds(place[groups[g][0]] * per, len(groups[g]) * per)
        result[at, :] = (mine[at, :] + part_in[at, :].astype(F32)).astype(BF16)
        for k in groups[g]:
            if k:
                giveback(k).start()
            else:
                returned[pl.ds(pl.multiple_of(me * per, per), per), :] = result[pl.ds(place[k] * per, per), :]

    for g in range(len(groups)):
        relay(g)
        if g:
            finish(g - 1)
        compute(g)
    finish(len(groups) - 1)

    ids_all = ids_ref[...]
    spots_all = lax.broadcasted_iota(jnp.int32, (tok, n * per), 0)
    combine = jnp.where(spots_all == ids_all, route_ref[...].astype(F32), 0.0).astype(BF16)
    for k in order:
        if k:
            giveback(k).wait_recv()
    out_ref[...] = jnp.dot(combine, returned[...], preferred_element_type=F32).astype(BF16)
    for k in order:
        if k:
            dispatch(k).wait_send()
            giveback(k).wait_send()
        forward(k).wait_send()
    for g in range(len(groups)):
        swap(g).wait_send()


def per_device(tokens, picks, route_weights, gate_weight, up_weight, down_weight):
    n = lax.axis_size("ep")
    experts, per = picks.shape
    tok, width = tokens.shape
    hidden = gate_weight.shape[2]
    slots, cols = n * per, width // 2
    groups = groups_of(n)
    local = picks - lax.axis_index("ep") * tok
    half_ids = local.reshape(n, 2, per // 2).transpose(1, 0, 2).reshape(2, slots // 2)
    any_spec, vmem_spec = pl.BlockSpec(memory_space=pl.ANY), pl.BlockSpec(memory_space=pltpu.VMEM)
    dma = pltpu.SemaphoreType.DMA
    return pl.pallas_call(
        functools.partial(kernel, n, per, groups),
        out_shape=jax.ShapeDtypeStruct((tok, cols), BF16),
        in_specs=[any_spec, vmem_spec, vmem_spec, vmem_spec, any_spec, any_spec, any_spec],
        out_specs=vmem_spec,
        scratch_shapes=[
            pltpu.VMEM((tok, width), BF16),
            pltpu.VMEM((width, hidden), BF16),
            pltpu.VMEM((width, hidden), BF16),
            pltpu.VMEM((hidden, width), BF16),
            pltpu.VMEM((slots // 2, width), BF16),
            pltpu.VMEM((slots, width), BF16),
            pltpu.VMEM((slots, cols), F32),
            pltpu.VMEM((slots, cols), BF16),
            pltpu.VMEM((slots, cols), BF16),
            pltpu.VMEM((slots, cols), BF16),
            pltpu.VMEM((slots, cols), BF16),
            dma((4,)),
            dma((n,)), dma((n,)), dma((n,)), dma((n,)),
            dma((len(groups),)), dma((len(groups),)),
            dma((n,)), dma((n,)),
        ],
        compiler_params=pltpu.CompilerParams(
            collective_id=0, has_side_effects=True, vmem_limit_bytes=60 * 1024 * 1024
        ),
    )(
        tokens, local.reshape(1, slots), half_ids, route_weights.reshape(1, slots),
        gate_weight, up_weight, down_weight,
    )


def solution(mesh):
    return jax.shard_map(
        per_device,
        mesh=mesh,
        in_specs=(
            P(("grp", "ep"), None),
            P(None, ("grp", "ep")),
            P(None, ("grp", "ep")),
            P("ep", None, "tp"),
            P("ep", None, "tp"),
            P("ep", "tp", None),
        ),
        out_specs=P(("grp", "ep"), "tp"),
        check_vma=False,
    )
```

```python
import functools

import jax
import jax.numpy as jnp
from jax import lax
from jax.experimental import pallas as pl
from jax.experimental.pallas import tpu as pltpu
from jax.sharding import PartitionSpec as P

MESH = pl.DeviceIdType.MESH
F32 = jnp.float32
BF16 = jnp.bfloat16


def flip(me, k):
    bit, out = 1, me
    while bit <= k:
        if k & bit:
            out = out + bit * (1 - 2 * ((me // bit) % 2))
        bit *= 2
    return out


def groups_of(n):
    if n < 4:
        return [list(range(n))]
    half, quarter = n // 2, n // 4
    return [
        list(range(half, half + quarter)),
        list(range(half)),
        list(range(half + quarter, n)),
    ]


def kernel(
    n, per, groups,
    tokens_hbm, picks_hbm, route_hbm, gate_hbm, up_hbm, down_hbm, returned, combine,
    tokens, picks, route, gate_w, up_w, down_w, outgoing, rows, mine, part_out, part_in, result,
    load_sem, disp_send, disp_recv, fwd_send, fwd_recv, part_send, part_recv, ret_send, ret_recv,
):
    me, core = lax.axis_index("ep"), lax.axis_index("tp")
    other = 1 - core
    half = per // 2
    tok, width = tokens.shape
    cols = width // 2
    order = [k for g in groups for k in g]
    place = {k: i for i, k in enumerate(order)}

    loads = [
        pltpu.make_async_copy(src, dst, load_sem.at[i])
        for i, (src, dst) in enumerate(
            (
                (picks_hbm, picks), (tokens_hbm, tokens), (route_hbm, route),
                (gate_hbm.at[0], gate_w), (up_hbm.at[0], up_w), (down_hbm.at[0], down_w),
            )
        )
    ]
    for load in loads:
        load.start()

    barrier = pltpu.get_barrier_semaphore()
    for k in order:
        if k:
            pl.semaphore_signal(barrier, inc=1, device_id={"ep": flip(me, k)}, device_id_type=MESH)
    pl.semaphore_signal(barrier, inc=1, device_id={"tp": other}, device_id_type=MESH)

    loads[0].wait()
    local = picks[...] - me * tok
    kept = jnp.where(core == 0, local[:, :half], local[:, half:])
    ids = jnp.concatenate([kept[e:e + 1, :] for e in range(n)], axis=1)
    spots = lax.broadcasted_iota(jnp.int32, (tok, n * half), 0)
    pick = jnp.where(spots == ids, 1.0, 0.0).astype(BF16)
    loads[1].wait()
    outgoing[...] = lax.dot_general(
        pick, tokens[...], (((0,), (0,)), ((), ())), preferred_element_type=F32
    ).astype(BF16)

    def spot(k):
        return pl.ds(place[k] * per + pl.multiple_of(core * half, half), half)

    def dispatch(k):
        peer = flip(me, k)
        return pltpu.make_async_remote_copy(
            outgoing.at[pl.ds(pl.multiple_of(peer * half, half), half)], rows.at[spot(k)],
            disp_send.at[k], disp_recv.at[k], device_id={"ep": peer}, device_id_type=MESH,
        )

    def forward(k):
        src = rows.at[spot(k)] if k else outgoing.at[pl.ds(pl.multiple_of(me * half, half), half)]
        return pltpu.make_async_remote_copy(
            src, rows.at[spot(k)], fwd_send.at[k], fwd_recv.at[k], device_id={"tp": other}, device_id_type=MESH,
        )

    def swap(g):
        at = pl.ds(place[groups[g][0]] * per, len(groups[g]) * per)
        return pltpu.make_async_remote_copy(
            part_out.at[at], part_in.at[at], part_send.at[g], part_recv.at[g],
            device_id={"tp": other}, device_id_type=MESH,
        )

    def giveback(k):
        return pltpu.make_async_remote_copy(
            result.at[pl.ds(place[k] * per, per)], returned.at[pl.ds(pl.multiple_of(me * per, per), per)],
            ret_send.at[k], ret_recv.at[k], device_id={"ep": flip(me, k)}, device_id_type=MESH,
        )

    pl.semaphore_wait(barrier, n)
    for k in order:
        if k:
            dispatch(k).start()
    forward(0).start()
    loads[2].wait()
    ids_all = jnp.concatenate([local[e:e + 1, :] for e in range(n)], axis=1)
    weight = route[...].astype(F32)
    weight_all = jnp.concatenate([weight[e:e + 1, :] for e in range(n)], axis=1)
    spots_all = lax.broadcasted_iota(jnp.int32, (tok, n * per), 0)
    combine[...] = jnp.where(spots_all == ids_all, weight_all, 0.0).astype(BF16)
    rows[spot(0), :] = outgoing[pl.ds(pl.multiple_of(me * half, half), half), :]

    def relay(g):
        for k in groups[g]:
            if k:
                dispatch(k).wait_recv()
                forward(k).start()

    def compute(g):
        for k in groups[g]:
            forward(k).wait_recv()
        if g == 0:
            for load in loads[3:]:
                load.wait()
        count = len(groups[g]) * per
        at = pl.ds(place[groups[g][0]] * per, count)
        x = rows[at, :]
        gate = jnp.dot(x, gate_w[...], preferred_element_type=F32)
        up = jnp.dot(x, up_w[...], preferred_element_type=F32)
        hidden = (gate / (1.0 + jnp.exp(-gate)) * up).astype(BF16)
        theirs = down_w[:, pl.ds(pl.multiple_of(other * cols, cols), cols)]
        part_out[at, :] = jnp.dot(hidden, theirs, preferred_element_type=F32).astype(BF16)
        swap(g).start()
        ours = down_w[:, pl.ds(pl.multiple_of(core * cols, cols), cols)]
        mine[at, :] = jnp.dot(hidden, ours, preferred_element_type=F32)

    def finish(g):
        swap(g).wait_recv()
        at = pl.ds(place[groups[g][0]] * per, len(groups[g]) * per)
        result[at, :] = (mine[at, :] + part_in[at, :].astype(F32)).astype(BF16)
        for k in groups[g]:
            if k:
                giveback(k).start()
            else:
                returned[pl.ds(pl.multiple_of(me * per, per), per), :] = result[pl.ds(place[k] * per, per), :]

    for g in range(len(groups)):
        relay(g)
        if g:
            finish(g - 1)
        compute(g)
    finish(len(groups) - 1)

    for k in order:
        if k:
            giveback(k).wait_recv()
    for k in order:
        if k:
            dispatch(k).wait_send()
            giveback(k).wait_send()
        forward(k).wait_send()
    for g in range(len(groups)):
        swap(g).wait_send()


def per_device(tokens, picks, route_weights, gate_weight, up_weight, down_weight):
    n = lax.axis_size("ep")
    experts, per = picks.shape
    tok, width = tokens.shape
    hidden = gate_weight.shape[2]
    slots, cols = n * per, width // 2
    groups = groups_of(n)
    any_spec, vmem_spec = pl.BlockSpec(memory_space=pl.ANY), pl.BlockSpec(memory_space=pltpu.VMEM)
    dma = pltpu.SemaphoreType.DMA
    returned, combine = pl.pallas_call(
        functools.partial(kernel, n, per, groups),
        out_shape=(
            jax.ShapeDtypeStruct((slots, cols), BF16), jax.ShapeDtypeStruct((tok, slots), BF16),
        ),
        in_specs=[any_spec] * 6,
        out_specs=(vmem_spec, vmem_spec),
        scratch_shapes=[
            pltpu.VMEM((tok, width), BF16),
            pltpu.VMEM((n, per), jnp.int32),
            pltpu.VMEM((n, per), BF16),
            pltpu.VMEM((width, hidden), BF16),
            pltpu.VMEM((width, hidden), BF16),
            pltpu.VMEM((hidden, width), BF16),
            pltpu.VMEM((slots // 2, width), BF16),
            pltpu.VMEM((slots, width), BF16),
            pltpu.VMEM((slots, cols), F32),
            pltpu.VMEM((slots, cols), BF16),
            pltpu.VMEM((slots, cols), BF16),
            pltpu.VMEM((slots, cols), BF16),
            dma((6,)),
            dma((n,)), dma((n,)), dma((n,)), dma((n,)),
            dma((len(groups),)), dma((len(groups),)),
            dma((n,)), dma((n,)),
        ],
        compiler_params=pltpu.CompilerParams(
            collective_id=0, has_side_effects=True, vmem_limit_bytes=60 * 1024 * 1024
        ),
    )(tokens, picks, route_weights, gate_weight, up_weight, down_weight)
    return jnp.dot(combine, returned, preferred_element_type=F32).astype(BF16)


def solution(mesh):
    return jax.shard_map(
        per_device,
        mesh=mesh,
        in_specs=(
            P(("grp", "ep"), None),
            P(None, ("grp", "ep")),
            P(None, ("grp", "ep")),
            P("ep", None, "tp"),
            P("ep", None, "tp"),
            P("ep", "tp", None),
        ),
        out_specs=P(("grp", "ep"), "tp"),
        check_vma=False,
    )
```

```python
import functools

import jax
import jax.numpy as jnp
from jax import lax
from jax.experimental import pallas as pl
from jax.experimental.pallas import tpu as pltpu
from jax.sharding import PartitionSpec as P

MESH = pl.DeviceIdType.MESH
F32 = jnp.float32
BF16 = jnp.bfloat16


def flip(me, k):
    bit, out = 1, me
    while bit <= k:
        if k & bit:
            out = out + bit * (1 - 2 * ((me // bit) % 2))
        bit *= 2
    return out


def groups_of(n):
    if n < 8:
        return [list(range(n))]
    half, eighth = n // 2, n // 8
    far = [list(range(at, at + eighth)) for at in range(half, n, eighth)]
    return far[:2] + [list(range(half))] + far[2:]


def kernel(
    n, per, groups,
    tokens_hbm, picks_hbm, route_hbm, gate_hbm, up_hbm, down_hbm, returned, combine,
    tokens, picks, route, gate_w, up_w, down_w, outgoing, rows, mine, part_out, part_in, result,
    load_sem, disp_send, disp_recv, fwd_send, fwd_recv, part_send, part_recv, ret_send, ret_recv,
):
    me, core = lax.axis_index("ep"), lax.axis_index("tp")
    other = 1 - core
    half = per // 2
    tok, width = tokens.shape
    cols = width // 2
    order = [k for g in groups for k in g]
    place = {k: i for i, k in enumerate(order)}

    loads = [
        pltpu.make_async_copy(src, dst, load_sem.at[i])
        for i, (src, dst) in enumerate(
            (
                (picks_hbm, picks), (tokens_hbm, tokens), (route_hbm, route),
                (gate_hbm.at[0], gate_w), (up_hbm.at[0], up_w), (down_hbm.at[0], down_w),
            )
        )
    ]
    for load in loads:
        load.start()

    barrier = pltpu.get_barrier_semaphore()
    for k in order:
        if k:
            pl.semaphore_signal(barrier, inc=1, device_id={"ep": flip(me, k)}, device_id_type=MESH)
    pl.semaphore_signal(barrier, inc=1, device_id={"tp": other}, device_id_type=MESH)

    loads[0].wait()
    spots = lax.broadcasted_iota(jnp.int32, (tok, n * half), 0)
    first = len(groups[0] + groups[1]) if len(groups) > 1 else n

    def gather(ks):
        kept = []
        for k in ks:
            row = picks[pl.ds(flip(me, k), 1), :] - me * tok
            kept.append(jnp.where(core == 0, row[:, :half], row[:, half:]))
        ids = jnp.concatenate(kept, axis=1)
        pick = jnp.where(spots[:, :len(ks) * half] == ids, 1.0, 0.0).astype(BF16)
        outgoing[pl.ds(place[ks[0]] * half, len(ks) * half), :] = lax.dot_general(
            pick, tokens[...], (((0,), (0,)), ((), ())), preferred_element_type=F32
        ).astype(BF16)

    loads[1].wait()
    gather(order[:first])

    def sent(k):
        return pl.ds(place[k] * half, half)

    def spot(k):
        return pl.ds(place[k] * per + pl.multiple_of(core * half, half), half)

    def dispatch(k):
        peer = flip(me, k)
        return pltpu.make_async_remote_copy(
            outgoing.at[sent(k)], rows.at[spot(k)],
            disp_send.at[k], disp_recv.at[k], device_id={"ep": peer}, device_id_type=MESH,
        )

    def forward(k):
        src = rows.at[spot(k)] if k else outgoing.at[sent(0)]
        return pltpu.make_async_remote_copy(
            src, rows.at[spot(k)], fwd_send.at[k], fwd_recv.at[k], device_id={"tp": other}, device_id_type=MESH,
        )

    def swap(g):
        at = pl.ds(place[groups[g][0]] * per, len(groups[g]) * per)
        return pltpu.make_async_remote_copy(
            part_out.at[at], part_in.at[at], part_send.at[g], part_recv.at[g],
            device_id={"tp": other}, device_id_type=MESH,
        )

    def giveback(k):
        return pltpu.make_async_remote_copy(
            result.at[pl.ds(place[k] * per, per)], returned.at[pl.ds(pl.multiple_of(me * per, per), per)],
            ret_send.at[k], ret_recv.at[k], device_id={"ep": flip(me, k)}, device_id_type=MESH,
        )

    pl.semaphore_wait(barrier, n)
    for k in order[:first]:
        if k:
            dispatch(k).start()
    if first < n:
        gather(order[first:])
        for k in order[first:]:
            if k:
                dispatch(k).start()
    forward(0).start()
    loads[2].wait()
    local = picks[...] - me * tok
    ids_all = jnp.concatenate([local[e:e + 1, :] for e in range(n)], axis=1)
    weight = route[...].astype(F32)
    weight_all = jnp.concatenate([weight[e:e + 1, :] for e in range(n)], axis=1)
    spots_all = lax.broadcasted_iota(jnp.int32, (tok, n * per), 0)
    combine[...] = jnp.where(spots_all == ids_all, weight_all, 0.0).astype(BF16)
    rows[spot(0), :] = outgoing[sent(0), :]

    def relay(g):
        for k in groups[g]:
            if k:
                dispatch(k).wait_recv()
                forward(k).start()

    def compute(g):
        for k in groups[g]:
            forward(k).wait_recv()
        if g == 0:
            for load in loads[3:]:
                load.wait()
        count = len(groups[g]) * per
        at = pl.ds(place[groups[g][0]] * per, count)
        x = rows[at, :]
        gate = jnp.dot(x, gate_w[...], preferred_element_type=F32)
        up = jnp.dot(x, up_w[...], preferred_element_type=F32)
        hidden = (gate / (1.0 + jnp.exp(-gate)) * up).astype(BF16)
        theirs = down_w[:, pl.ds(pl.multiple_of(other * cols, cols), cols)]
        part_out[at, :] = jnp.dot(hidden, theirs, preferred_element_type=F32).astype(BF16)
        swap(g).start()
        ours = down_w[:, pl.ds(pl.multiple_of(core * cols, cols), cols)]
        mine[at, :] = jnp.dot(hidden, ours, preferred_element_type=F32)

    def finish(g):
        swap(g).wait_recv()
        at = pl.ds(place[groups[g][0]] * per, len(groups[g]) * per)
        result[at, :] = (mine[at, :] + part_in[at, :].astype(F32)).astype(BF16)
        for k in groups[g]:
            if k:
                giveback(k).start()
            else:
                returned[pl.ds(pl.multiple_of(me * per, per), per), :] = result[pl.ds(place[k] * per, per), :]

    for g in range(len(groups)):
        relay(g)
        if g:
            finish(g - 1)
        compute(g)
    finish(len(groups) - 1)

    for k in order:
        if k:
            giveback(k).wait_recv()
    for k in order:
        if k:
            dispatch(k).wait_send()
            giveback(k).wait_send()
        forward(k).wait_send()
    for g in range(len(groups)):
        swap(g).wait_send()


def per_device(tokens, picks, route_weights, gate_weight, up_weight, down_weight):
    n = lax.axis_size("ep")
    experts, per = picks.shape
    tok, width = tokens.shape
    hidden = gate_weight.shape[2]
    slots, cols = n * per, width // 2
    groups = groups_of(n)
    any_spec, vmem_spec = pl.BlockSpec(memory_space=pl.ANY), pl.BlockSpec(memory_space=pltpu.VMEM)
    dma = pltpu.SemaphoreType.DMA
    returned, combine = pl.pallas_call(
        functools.partial(kernel, n, per, groups),
        out_shape=(
            pltpu.VMEM((slots, cols), BF16), pltpu.VMEM((tok, slots), BF16),
        ),
        in_specs=[any_spec] * 6,
        out_specs=(vmem_spec, vmem_spec),
        scratch_shapes=[
            pltpu.VMEM((tok, width), BF16),
            pltpu.VMEM((n, per), jnp.int32),
            pltpu.VMEM((n, per), BF16),
            pltpu.VMEM((width, hidden), BF16),
            pltpu.VMEM((width, hidden), BF16),
            pltpu.VMEM((hidden, width), BF16),
            pltpu.VMEM((slots // 2, width), BF16),
            pltpu.VMEM((slots, width), BF16),
            pltpu.VMEM((slots, cols), F32),
            pltpu.VMEM((slots, cols), BF16),
            pltpu.VMEM((slots, cols), BF16),
            pltpu.VMEM((slots, cols), BF16),
            dma((6,)),
            dma((n,)), dma((n,)), dma((n,)), dma((n,)),
            dma((len(groups),)), dma((len(groups),)),
            dma((n,)), dma((n,)),
        ],
        compiler_params=pltpu.CompilerParams(
            collective_id=0, has_side_effects=True, vmem_limit_bytes=60 * 1024 * 1024
        ),
    )(tokens, picks, route_weights, gate_weight, up_weight, down_weight)
    return jnp.dot(combine, returned, preferred_element_type=F32).astype(BF16)


def solution(mesh):
    return jax.shard_map(
        per_device,
        mesh=mesh,
        in_specs=(
            P(("grp", "ep"), None),
            P(None, ("grp", "ep")),
            P(None, ("grp", "ep")),
            P("ep", None, "tp"),
            P("ep", None, "tp"),
            P("ep", "tp", None),
        ),
        out_specs=P(("grp", "ep"), "tp"),
        check_vma=False,
    )
```

```python
import functools

import jax
import jax.numpy as jnp
from jax import lax
from jax.experimental import pallas as pl
from jax.experimental.pallas import tpu as pltpu
from jax.sharding import PartitionSpec as P

MESH = pl.DeviceIdType.MESH
F32 = jnp.float32
BF16 = jnp.bfloat16


def flip(me, k):
    bit, out = 1, me
    while bit <= k:
        if k & bit:
            out = out + bit * (1 - 2 * ((me // bit) % 2))
        bit *= 2
    return out


def groups_of(n):
    if n < 8:
        return [list(range(n))], [[]], list(range(n))
    half, quarter, eighth = n // 2, n // 4, n // 8
    far = [list(range(at, at + eighth)) for at in range(half, n, eighth)]
    far = far[2:] + far[:2]
    nearest, near = list(range(quarter)), list(range(quarter, half))
    groups = [nearest, far[0], far[1], near, far[2], far[3]]
    return groups, [[1], [2], [3], [4, 5], [], []], far[0] + far[1] + nearest + near + far[2] + far[3]


def kernel(
    n, per, groups, ahead, sending,
    tokens_hbm, picks_hbm, route_hbm, gate_hbm, up_hbm, down_hbm, returned, combine,
    tokens, picks, route, gate_w, up_w, down_w, outgoing, rows, mine, part_out, part_in, result,
    load_sem, disp_send, disp_recv, fwd_send, fwd_recv, part_send, part_recv, ret_send, ret_recv,
):
    me, core = lax.axis_index("ep"), lax.axis_index("tp")
    other = 1 - core
    half = per // 2
    tok, width = tokens.shape
    cols = width // 2
    order = [k for g in groups for k in g]
    place = {k: i for i, k in enumerate(order)}

    loads = [
        pltpu.make_async_copy(src, dst, load_sem.at[i])
        for i, (src, dst) in enumerate(
            (
                (picks_hbm, picks), (tokens_hbm, tokens), (route_hbm, route),
                (gate_hbm.at[0], gate_w), (up_hbm.at[0], up_w), (down_hbm.at[0], down_w),
            )
        )
    ]
    for load in loads:
        load.start()

    barrier = pltpu.get_barrier_semaphore()
    for k in order:
        if k:
            pl.semaphore_signal(barrier, inc=1, device_id={"ep": flip(me, k)}, device_id_type=MESH)
    pl.semaphore_signal(barrier, inc=1, device_id={"tp": other}, device_id_type=MESH)

    loads[0].wait()
    spots = lax.broadcasted_iota(jnp.int32, (tok, n * half), 0)
    first = len(groups[0] + groups[1] + groups[2]) if len(groups) > 1 else n

    def gather(ks):
        kept = []
        for k in ks:
            row = picks[pl.ds(flip(me, k), 1), :] - me * tok
            kept.append(jnp.where(core == 0, row[:, :half], row[:, half:]))
        ids = jnp.concatenate(kept, axis=1)
        pick = jnp.where(spots[:, :len(ks) * half] == ids, 1.0, 0.0).astype(BF16)
        outgoing[pl.ds(place[ks[0]] * half, len(ks) * half), :] = lax.dot_general(
            pick, tokens[...], (((0,), (0,)), ((), ())), preferred_element_type=F32
        ).astype(BF16)

    loads[1].wait()
    gather(order[:first])

    def sent(k):
        return pl.ds(place[k] * half, half)

    def spot(k):
        return pl.ds(place[k] * per + pl.multiple_of(core * half, half), half)

    def dispatch(k):
        peer = flip(me, k)
        return pltpu.make_async_remote_copy(
            outgoing.at[sent(k)], rows.at[spot(k)],
            disp_send.at[k], disp_recv.at[k], device_id={"ep": peer}, device_id_type=MESH,
        )

    def forward(k):
        src = rows.at[spot(k)] if k else outgoing.at[sent(0)]
        return pltpu.make_async_remote_copy(
            src, rows.at[spot(k)], fwd_send.at[k], fwd_recv.at[k], device_id={"tp": other}, device_id_type=MESH,
        )

    def swap(g):
        at = pl.ds(place[groups[g][0]] * per, len(groups[g]) * per)
        return pltpu.make_async_remote_copy(
            part_out.at[at], part_in.at[at], part_send.at[g], part_recv.at[g],
            device_id={"tp": other}, device_id_type=MESH,
        )

    def giveback(k):
        return pltpu.make_async_remote_copy(
            result.at[pl.ds(place[k] * per, per)], returned.at[pl.ds(pl.multiple_of(me * per, per), per)],
            ret_send.at[k], ret_recv.at[k], device_id={"ep": flip(me, k)}, device_id_type=MESH,
        )

    pl.semaphore_wait(barrier, n)
    for k in sending[:first]:
        if k:
            dispatch(k).start()
    if first < n:
        gather(order[first:])
        for k in sending[first:]:
            dispatch(k).start()
    forward(0).start()
    loads[2].wait()
    local = picks[...] - me * tok
    ids_all = jnp.concatenate([local[e:e + 1, :] for e in range(n)], axis=1)
    weight = route[...].astype(F32)
    weight_all = jnp.concatenate([weight[e:e + 1, :] for e in range(n)], axis=1)
    spots_all = lax.broadcasted_iota(jnp.int32, (tok, n * per), 0)
    combine[...] = jnp.where(spots_all == ids_all, weight_all, 0.0).astype(BF16)
    rows[spot(0), :] = outgoing[sent(0), :]

    def relay(g):
        for k in groups[g]:
            if k:
                dispatch(k).wait_recv()
                forward(k).start()

    def region(g):
        return pl.ds(place[groups[g][0]] * per, len(groups[g]) * per)

    def enter(g):
        for k in groups[g]:
            forward(k).wait_recv()
        x = rows[region(g), :]
        if g == 0:
            loads[3].wait()
        gate = jnp.dot(x, gate_w[...], preferred_element_type=F32)
        if g == 0:
            loads[4].wait()
        up = jnp.dot(x, up_w[...], preferred_element_type=F32)
        return (gate / (1.0 + jnp.exp(-gate)) * up).astype(BF16)

    def leave(g, hidden):
        if g == 0:
            loads[5].wait()
        theirs = down_w[:, pl.ds(pl.multiple_of(other * cols, cols), cols)]
        part_out[region(g), :] = jnp.dot(hidden, theirs, preferred_element_type=F32).astype(BF16)
        swap(g).start()
        ours = down_w[:, pl.ds(pl.multiple_of(core * cols, cols), cols)]
        mine[region(g), :] = jnp.dot(hidden, ours, preferred_element_type=F32)

    def finish(g):
        swap(g).wait_recv()
        at = pl.ds(place[groups[g][0]] * per, len(groups[g]) * per)
        result[at, :] = (mine[at, :] + part_in[at, :].astype(F32)).astype(BF16)
        for k in groups[g]:
            if k:
                giveback(k).start()
            else:
                returned[pl.ds(pl.multiple_of(me * per, per), per), :] = result[pl.ds(place[k] * per, per), :]

    relay(0)
    for g in range(len(groups)):
        hidden = enter(g)
        for later in ahead[g]:
            relay(later)
        if g:
            finish(g - 1)
        leave(g, hidden)
    finish(len(groups) - 1)

    for k in order:
        if k:
            giveback(k).wait_recv()
    for k in order:
        if k:
            dispatch(k).wait_send()
            giveback(k).wait_send()
        forward(k).wait_send()
    for g in range(len(groups)):
        swap(g).wait_send()


def per_device(tokens, picks, route_weights, gate_weight, up_weight, down_weight):
    n = lax.axis_size("ep")
    experts, per = picks.shape
    tok, width = tokens.shape
    hidden = gate_weight.shape[2]
    slots, cols = n * per, width // 2
    groups, ahead, sending = groups_of(n)
    any_spec, vmem_spec = pl.BlockSpec(memory_space=pl.ANY), pl.BlockSpec(memory_space=pltpu.VMEM)
    dma = pltpu.SemaphoreType.DMA
    returned, combine = pl.pallas_call(
        functools.partial(kernel, n, per, groups, ahead, sending),
        out_shape=(
            pltpu.VMEM((slots, cols), BF16), pltpu.VMEM((tok, slots), BF16),
        ),
        in_specs=[any_spec] * 6,
        out_specs=(vmem_spec, vmem_spec),
        scratch_shapes=[
            pltpu.VMEM((tok, width), BF16),
            pltpu.VMEM((n, per), jnp.int32),
            pltpu.VMEM((n, per), BF16),
            pltpu.VMEM((width, hidden), BF16),
            pltpu.VMEM((width, hidden), BF16),
            pltpu.VMEM((hidden, width), BF16),
            pltpu.VMEM((slots // 2, width), BF16),
            pltpu.VMEM((slots, width), BF16),
            pltpu.VMEM((slots, cols), F32),
            pltpu.VMEM((slots, cols), BF16),
            pltpu.VMEM((slots, cols), BF16),
            pltpu.VMEM((slots, cols), BF16),
            dma((6,)),
            dma((n,)), dma((n,)), dma((n,)), dma((n,)),
            dma((len(groups),)), dma((len(groups),)),
            dma((n,)), dma((n,)),
        ],
        compiler_params=pltpu.CompilerParams(
            collective_id=0, has_side_effects=True, vmem_limit_bytes=60 * 1024 * 1024
        ),
    )(tokens, picks, route_weights, gate_weight, up_weight, down_weight)
    return jnp.dot(combine, returned, preferred_element_type=F32).astype(BF16)


def solution(mesh):
    return jax.shard_map(
        per_device,
        mesh=mesh,
        in_specs=(
            P(("grp", "ep"), None),
            P(None, ("grp", "ep")),
            P(None, ("grp", "ep")),
            P("ep", None, "tp"),
            P("ep", None, "tp"),
            P("ep", "tp", None),
        ),
        out_specs=P(("grp", "ep"), "tp"),
        check_vma=False,
    )
```
